32 devices in a mesh: ra: 4 (over z), cb: 4 (over y, x), dp: 2 (over core).
Axes of the slice: x: 2, y: 2, z: 4, core: 2. Of those that a mesh axis runs over, the one named last changes fastest.
Arguments:
- tokens: bfloat16 [3072, 4096], P('dp', 'ra'), may hold values from -20 to 20
- pre_gain: float32 [4096], P('ra'), may hold values from 0.1 to 1.9
- up_weight: bfloat16 [4096, 16384], P('ra', 'cb'), may hold values from -0.09375 to 0.09375
- up_bias: float32 [16384], P('cb'), may hold values from -4 to 4
- down_weight: bfloat16 [16384, 4096], P('cb', 'ra'), may hold values from -0.046875 to 0.046875
- post_gain: float32 [4096], P('ra'), may hold values from 0.1 to 1.9
Outputs:
- stream_out: bfloat16 [3072, 4096], P('dp', 'ra')
The draws below stay inside these ranges and needn't reach their ends.
All inputs are finite; a program needn't handle non-finite values.
Results may differ from the reference program's by a relative error of at most 0.0051.
Values may be sent and summed in bfloat16 or wider, within the bound.
No kernel may reach another device: no remote copies, remote signals or barrier semaphores. Data moves between devices by JAX's collectives and lax.ppermute only.
A program may use at most 128 MiB of HBM per device.

```python
import jax
import jax.numpy as jnp
from jax import lax

D = 4096
FF = 16384
TOKENS = 3072


def draw_tokens(key, part):
    first, second, third = jax.random.split(key, 3)
    column = jnp.exp(jax.random.uniform(second, (D // 16,), jnp.float32, -1.2, 1.2))
    column = jnp.repeat(column, 16)
    values = jax.random.normal(first, (TOKENS, D), jnp.float32) * column
    return jnp.clip(values, -20.0, 20.0).astype(jnp.bfloat16)


def block_scale(rng, shape, cuts, low, largest):
    gain = 1.0
    for axis_at, shards_of in cuts:
        draws = jax.random.uniform(jax.random.fold_in(jax.random.fold_in(rng, 6), axis_at), (shards_of,), jnp.float32, low / len(cuts), largest / len(cuts))
        gain = gain * jnp.repeat(jnp.exp(draws), shape[axis_at] // shards_of).reshape((-1,) + (1,) * (len(shape) - 1 - axis_at))
    return gain


def bell_draw(own_key, shape, deviation, limit, shards=(), held_as=jnp.bfloat16):
    drawn = jax.random.normal(own_key, shape, jnp.float32) * deviation
    if len(shards) > 0:
        drawn = block_scale(own_key, shape, shards, -0.22, 0.18) * drawn
    return jnp.clip(drawn, min=-limit, max=limit).astype(held_as)


def setup_inputs(seed: int = 0) -> dict:
    seeds = jax.random.split(jax.random.key(seed), 7)
    return {
        "tokens": draw_tokens(jax.random.fold_in(seeds[6], 71), 0),
        "pre_gain": jnp.clip(1.0 + 0.18 * jax.random.normal(seeds[1], (D,), jnp.float32), 0.1, 1.9),
        "up_weight": bell_draw(seeds[2], (D, FF), D ** -0.5, 0.09375, ((0, 4), (1, 4))),
        "up_bias": bell_draw(seeds[3], (FF,), 1.0, 4.0, ((0, 4),), jnp.float32),
        "down_weight": bell_draw(seeds[4], (FF, D), FF ** -0.5, 0.046875, ((0, 4), (1, 4))),
        "post_gain": jnp.clip(1.0 + 0.18 * jax.random.normal(seeds[5], (D,), jnp.float32), 0.1, 1.9),
    }


epsilon = 1e-06
residual_weight = 0.5

def reference(tokens, pre_gain, up_weight, up_bias, down_weight, post_gain):
    stream = tokens.astype(jnp.float32)
    energy = lax.optimization_barrier(jnp.sum(stream * stream, axis=1))
    inverse = lax.rsqrt(energy / D + epsilon)
    scaled = (stream * pre_gain).astype(jnp.bfloat16)
    pre = jnp.dot(scaled, up_weight, preferred_element_type=jnp.float32) * inverse[:, None] + up_bias
    hidden = jnp.square(jax.nn.relu(pre)).astype(jnp.bfloat16)
    branch = jnp.dot(hidden, down_weight, preferred_element_type=jnp.float32)
    branch_energy = lax.optimization_barrier(jnp.sum(branch * branch, axis=1))
    normed = branch * lax.rsqrt(branch_energy / D + epsilon)[:, None] * post_gain
    return (residual_weight * stream + normed).astype(jnp.bfloat16)
```

```python
import jax
import jax.numpy as jnp
from jax import lax
from jax.sharding import PartitionSpec as P

epsilon = 1e-06
residual_weight = 0.5
CHUNKS = 8
GROUP = 3


def divisor_at_most(total, wanted):
    count = min(wanted, total)
    while total % count:
        count -= 1
    return count


def line_sum(value, axis, size):
    if size > 4:
        return lax.psum(value, axis)
    parts = [value]
    for shift in range(1, size):
        parts.append(lax.ppermute(value, axis, [(i, (i + shift) % size) for i in range(size)]))
    total = parts[0]
    for part in parts[1:]:
        total = total + part
    return total


def body(ra_size, cb_size, tokens, pre_gain, up_weight, up_bias, down_weight, post_gain):
    last = ra_size - 1
    z = lax.axis_index("ra")
    rows, width = tokens.shape
    features = width * ra_size
    half = rows // 2
    chunks = divisor_at_most(half, CHUNKS)
    r = half // chunks
    steps = chunks + 2 * last

    stream = tokens.astype(jnp.float32)
    energy = line_sum(jnp.sum(stream * stream, axis=1), "ra", ra_size)
    inverse = lax.rsqrt(energy / features + epsilon)

    def take(array, start):
        return lax.dynamic_slice_in_dim(array, start, r, 0)

    def product(t):
        low = jnp.clip(t - (last - z), 0, chunks - 1) * r
        high = half + jnp.clip(t - z, 0, chunks - 1) * r
        both = jnp.concatenate([take(tokens, low), take(tokens, high)], axis=0)
        scaled = (both.astype(jnp.float32) * pre_gain).astype(jnp.bfloat16)
        partial = jnp.dot(scaled, up_weight, preferred_element_type=jnp.float32)
        scale = jnp.concatenate([take(inverse, low), take(inverse, high)], axis=0)
        return partial, scale

    def valid(index):
        return 0 <= index < chunks

    def activate(summed, scale):
        return jnp.square(jax.nn.relu(summed * scale[:, None] + up_bias)).astype(jnp.bfloat16)

    def exchange(value):
        total = value.astype(jnp.float32)
        bit = 1
        while bit < cb_size:
            sent = total.astype(jnp.bfloat16)
            got = lax.ppermute(sent, "cb", [(i, i ^ bit) for i in range(cb_size)])
            total = sent.astype(jnp.float32) + got.astype(jnp.float32)
            bit *= 2
        return total

    sums = []
    pending = []
    down_sum = up_sum = None
    up_hidden = down_hidden = None
    for t in range(steps):
        act_low = act_high = None
        if t < chunks + last:
            partial, scale = product(t)
            low, high = partial[:r], partial[r:]
            if down_sum is not None:
                low = low + down_sum.astype(jnp.float32)
                high = high + up_sum.astype(jnp.float32)
            pairs_down = [(i, i - 1) for i in range(1, ra_size) if valid(t - (last - i))]
            pairs_up = [(i, i + 1) for i in range(last) if valid(t - i)]
            if pairs_down:
                down_sum = lax.ppermute(low.astype(jnp.bfloat16), "ra", pairs_down)
            if pairs_up:
                up_sum = lax.ppermute(high.astype(jnp.bfloat16), "ra", pairs_up)
            if t >= last:
                act_low = activate(low, scale[:r])
                act_high = activate(high, scale[r:])
        if t >= last:
            hidden_low, hidden_high = act_low, act_high
            if up_hidden is not None:
                if act_low is None:
                    hidden_low, hidden_high = up_hidden, down_hidden
                else:
                    hidden_low = jnp.where(z == 0, act_low, up_hidden)
                    hidden_high = jnp.where(z == last, act_high, down_hidden)
            pairs_up = [(i, i + 1) for i in range(last) if valid(t - last - i)]
            pairs_down = [(i, i - 1) for i in range(1, ra_size) if valid(t - last - (last - i))]
            if pairs_up:
                up_hidden = lax.ppermute(hidden_low, "ra", pairs_up)
            if pairs_down:
                down_hidden = lax.ppermute(hidden_high, "ra", pairs_down)
            branch = jnp.dot(
                jnp.concatenate([hidden_low, hidden_high], axis=0),
                down_weight,
                preferred_element_type=jnp.float32,
            )
            pending.append(branch.astype(jnp.bfloat16))
            if len(pending) == GROUP or t == steps - 1:
                total = exchange(jnp.concatenate(pending, axis=0))
                power = jnp.sum(total * total, axis=1)
                for i in range(len(pending)):
                    at = 2 * r * i
                    sums.append((total[at:at + r], power[at:at + r], total[at + r:at + 2 * r], power[at + r:at + 2 * r]))
                pending = []

    def gather(column, start):
        whole = jnp.concatenate([s[column] for s in sums], axis=0)
        return lax.dynamic_slice_in_dim(whole, start * r, half, 0)

    branch = jnp.concatenate([gather(0, z), gather(2, last - z)], axis=0)
    power = jnp.concatenate([gather(1, z), gather(3, last - z)], axis=0)
    branch_energy = line_sum(power, "ra", ra_size)
    normed = branch * lax.rsqrt(branch_energy / features + epsilon)[:, None] * post_gain
    return (residual_weight * stream + normed).astype(jnp.bfloat16)


def solution(mesh):
    ra_size, cb_size = mesh.shape["ra"], mesh.shape["cb"]

    def local(*arrays):
        return body(ra_size, cb_size, *arrays)

    in_specs = (P("dp", "ra"), P("ra"), P("ra", "cb"), P("cb"), P("cb", "ra"), P("ra"))
    return jax.shard_map(local, mesh=mesh, in_specs=in_specs, out_specs=P("dp", "ra"), check_vma=False)
```
